128 devices in a mesh: ep: 32 (over z, y, core), tp: 4 (over x).
Axes of the slice: x: 4, y: 4, z: 4, core: 2. Of those that a mesh axis runs over, the one named last changes fastest.
Arguments:
- query_rows: bfloat16 [16384, 1024], P('ep', 'tp'), may hold values from -60 to 60
- key_rows: bfloat16 [16384, 1024], P('ep', 'tp'), may hold values from -6 to 6
- value_rows: bfloat16 [16384, 1024], P('ep', 'tp'), may hold values from -6 to 6
- lambdas: float32 [8], P('tp'), may hold values from 0.3 to 0.8
- out_gain: float32 [128], replicated, may hold values from 0.1 to 1.9
- out_weight: bfloat16 [1024, 2048], P('tp'), may hold values from -0.1875 to 0.1875
- tokens: bfloat16 [16384, 2048], P(('ep', 'tp')), may hold values from -6 to 6
- norm_gain: float32 [2048], replicated, may hold values from 0.1 to 1.9
- group_ids: int32 [16384], P(('ep', 'tp')), may hold values from 0 to 3, as said below
- inner_ids: int32 [16384, 2], P(('ep', 'tp')), may hold values from 0 to 7, as said below
- route_weights: float32 [16384, 2], P(('ep', 'tp')), may hold values from 0.2 to 1
- gate_weight: bfloat16 [32, 2048, 1024], P('ep', None, 'tp'), may hold values from -0.125 to 0.125
- up_weight: bfloat16 [32, 2048, 1024], P('ep', None, 'tp'), may hold values from -0.125 to 0.125
- down_weight: bfloat16 [32, 1024, 2048], P('ep', 'tp'), may hold values from -0.1875 to 0.1875
Outputs:
- attended: bfloat16 [16384, 2048], P(('ep', 'tp'))
- combined: bfloat16 [16384, 2048], P(('ep', 'tp'))
The draws below stay inside these ranges and needn't reach their ends.
Inputs may be any that keep to these rules, and one draw needn't show every extreme that they name: In the 128 rows of one device no expert group_ids * 8 + inner_ids is named more than 10 times; some expert is named exactly 10 times in the rows of every device. `inner_ids`: the 2 entries of a row are different.
All inputs are finite; a program needn't handle non-finite values.
Results may differ from the reference program's by a relative error of at most 0.013.
Values may be sent and summed in bfloat16 or wider, within the bound.
No kernel may reach another device: no remote copies, remote signals or barrier semaphores. Data moves between devices by JAX's collectives and lax.ppermute only.
A program may use at most 128 MiB of HBM per device.

```python
import jax
import jax.numpy as jnp
from jax import lax

D = 2048
HEADS = 8
DQ = 64
DV = 128
FF = 1024
GROUPS = 4
TOPK = 2
TOK_DEV = 128
SEG = 512
TOKENS = 16384
EXPERTS = 32
CAP = 10
N_EP = 32
N_TP = 4


def paired_scores(base_key):
    width_cols = HEADS * 2 * DQ
    query_base = jnp.clip(jax.random.normal(jax.random.fold_in(base_key, 21), (TOKENS, width_cols), jnp.float32), -4.5, 4.5) * 1.3
    key_base = jnp.clip(jax.random.normal(jax.random.fold_in(base_key, 22), (TOKENS, width_cols), jnp.float32), -4.5, 4.5) * 1.3
    return (query_base, key_base)


def draw_query_rows(key, part):
    return paired_scores(key)[0].astype(jnp.bfloat16)


def draw_key_rows(key, part):
    return paired_scores(key)[1].astype(jnp.bfloat16)


def route_cells(base_key):
    group_size = EXPERTS // GROUPS
    per_row = group_size // TOPK
    per_group = CAP * per_row
    blocks = TOKENS // TOK_DEV
    hot = jax.random.randint(jax.random.fold_in(base_key, 31), (), 0, GROUPS).astype(jnp.int32)

    def one_block(block_num):
        block_key = jax.random.fold_in(jax.random.fold_in(base_key, 32), block_num)
        spare = jax.random.permutation(jax.random.fold_in(block_key, 1), (GROUPS - 1) * per_group)
        spare = spare[:TOK_DEV - per_group].astype(jnp.int32)
        spare_group = spare // per_group
        spare_group = spare_group + (spare_group >= hot).astype(jnp.int32)
        cell_group = jnp.concatenate([jnp.zeros((per_group,), jnp.int32) + hot, spare_group])
        cell_local = jnp.concatenate([jnp.arange(per_group, dtype=jnp.int32), spare % per_group])
        order = jax.random.permutation(jax.random.fold_in(block_key, 2), TOK_DEV).astype(jnp.int32)
        tok_group = cell_group[order]
        tok_local = cell_local[order]
        row_of = tok_group * CAP + tok_local // per_row
        slot_num = tok_local % per_row
        scores = jax.random.randint(jax.random.fold_in(block_key, 3), (GROUPS * CAP, group_size), 0, 1 << 20)
        scores = scores * group_size + jnp.arange(group_size, dtype=jnp.int32)[None, :]
        shuffle = jnp.argsort(scores, axis=1).astype(jnp.int32)
        columns = slot_num[:, None] * TOPK + jnp.arange(TOPK, dtype=jnp.int32)[None, :]
        chosen = jnp.take_along_axis(shuffle[row_of], columns, axis=1)
        return (tok_group, chosen)
    groups_all, inner_all = jax.vmap(one_block)(jnp.arange(blocks, dtype=jnp.int32))
    return (groups_all.reshape(TOKENS).astype(jnp.int32), inner_all.reshape(TOKENS, TOPK).astype(jnp.int32))


def draw_group_ids(key, part):
    return route_cells(key)[0]


def draw_inner_ids(key, part):
    return route_cells(key)[1]


def level_of(stream_key, shape, split, least, top_value):
    level, own = 1.0, jax.random.fold_in(stream_key, 6)
    for axis_at, parts in split:
        draws = jnp.exp(jax.random.uniform(jax.random.fold_in(own, axis_at), (parts,), jnp.float32, least / len(split), top_value / len(split)))
        level = level * jnp.repeat(draws, shape[axis_at] // parts).reshape([-1 if axis == axis_at else 1 for axis in range(len(shape))])
    return level


def normal_values(stream_key, extent, scale, bound, cuts=(), kind=jnp.bfloat16):
    values = jax.random.normal(stream_key, extent, jnp.float32) * scale
    if len(cuts) > 0:
        values = level_of(stream_key, extent, cuts, -0.22, 0.18) * values
    return jnp.clip(values, min=-bound, max=bound).astype(kind)


def setup_inputs(seed: int = 0) -> dict:
    keys = jax.random.split(jax.random.key(seed), 15)
    query_rows = draw_query_rows(jax.random.fold_in(keys[14], 71), 0)
    key_rows = draw_key_rows(jax.random.fold_in(keys[14], 71), 0)
    value_rows = normal_values(keys[2], (TOKENS, HEADS * DV), 1.0, 6.0, ((0, 32), (1, 4)))
    lambdas = jnp.clip(0.3 + 0.5 * jax.random.uniform(keys[3], (HEADS,), jnp.float32) ** level_of(keys[3], (HEADS,), ((0, 4),), -0.2, 0.2), 0.3, 0.8)
    out_gain = jnp.clip(1.0 + 0.18 * jax.random.normal(keys[4], (DV,), jnp.float32), 0.1, 1.9)
    out_weight = normal_values(keys[5], (HEADS * DV, D), (HEADS * DV) ** -0.5, 0.1875, ((0, 4),))
    tokens = normal_values(keys[6], (TOKENS, D), 1.0, 6.0, ((0, 128),))
    norm_gain = jnp.clip(1.0 + 0.18 * jax.random.normal(keys[7], (D,), jnp.float32), 0.1, 1.9)
    group_ids = draw_group_ids(jax.random.fold_in(keys[14], 71), 0)
    inner_ids = draw_inner_ids(jax.random.fold_in(keys[14], 71), 0)
    route_weights = jnp.clip(0.2 + 0.8 * jax.random.uniform(keys[10], (TOKENS, TOPK), jnp.float32) ** level_of(keys[10], (TOKENS, TOPK), ((0, 128),), -0.2, 0.2), 0.2, 1.0)
    gate_weight = normal_values(keys[11], (EXPERTS, D, FF), D ** -0.5, 0.125, ((0, 32), (2, 4)))
    up_weight = normal_values(keys[12], (EXPERTS, D, FF), D ** -0.5, 0.125, ((0, 32), (2, 4)))
    down_weight = normal_values(keys[13], (EXPERTS, FF, D), FF ** -0.5, 0.1875, ((0, 32), (1, 4)))
    return dict(query_rows=query_rows, key_rows=key_rows, value_rows=value_rows, lambdas=lambdas, out_gain=out_gain, out_weight=out_weight, tokens=tokens, norm_gain=norm_gain, group_ids=group_ids, inner_ids=inner_ids, route_weights=route_weights, gate_weight=gate_weight, up_weight=up_weight, down_weight=down_weight)


eps = 1e-06

def one_map(query_part, key_all, value_all, allowed):
    scores = jnp.dot(query_part, key_all.T, preferred_element_type=jnp.float32) * DQ ** (-0.5)
    scores = jnp.where(allowed, scores, -jnp.inf)
    row_top = lax.optimization_barrier(jnp.max(scores, axis=1, keepdims=True))
    exps = jnp.exp(scores - row_top)
    totals = lax.optimization_barrier(jnp.sum(exps, axis=1, keepdims=True))
    weighted = jnp.dot(exps.astype(jnp.bfloat16), value_all, preferred_element_type=jnp.float32)
    return weighted / totals

def head_output(operands):
    query_head, key_head, value_head, lambda_head = operands
    key_pos = jnp.arange(TOKENS, dtype=jnp.int32)

    def query_block(block_num):
        first_row = block_num * SEG
        query_part = lax.dynamic_slice_in_dim(query_head, first_row, SEG, 0)
        query_pos = first_row + jnp.arange(SEG, dtype=jnp.int32)
        allowed = key_pos[None, :] <= query_pos[:, None]
        first_map = one_map(query_part[:, 0], key_head[:, 0], value_head, allowed)
        second_map = one_map(query_part[:, 1], key_head[:, 1], value_head, allowed)
        heads_out = first_map - lambda_head * second_map
        mean_sq = lax.optimization_barrier(jnp.mean(heads_out * heads_out, axis=1, keepdims=True))
        return heads_out * lax.rsqrt(mean_sq + eps)
    return lax.map(query_block, jnp.arange(N_EP, dtype=jnp.int32)).reshape(TOKENS, DV)

def reference(query_rows, key_rows, value_rows, lambdas, out_gain, out_weight, tokens, norm_gain, group_ids, inner_ids, route_weights, gate_weight, up_weight, down_weight):
    query_heads = query_rows.reshape(TOKENS, HEADS, 2, DQ).transpose(1, 0, 2, 3)
    key_heads = key_rows.reshape(TOKENS, HEADS, 2, DQ).transpose(1, 0, 2, 3)
    value_heads = value_rows.reshape(TOKENS, HEADS, DV).transpose(1, 0, 2)
    per_head = lax.map(head_output, (query_heads, key_heads, value_heads, lambdas))
    normed_heads = (per_head * out_gain).astype(jnp.bfloat16).transpose(1, 0, 2).reshape(TOKENS, HEADS * DV)
    attended = jnp.dot(normed_heads, out_weight, preferred_element_type=jnp.float32).astype(jnp.bfloat16)
    tok_wide = tokens.astype(jnp.float32)
    normed = (tok_wide * lax.rsqrt(lax.optimization_barrier(jnp.mean(tok_wide * tok_wide, axis=1, keepdims=True)) + eps) * norm_gain).astype(jnp.bfloat16)
    picks = (group_ids[:, None] * (EXPERTS // GROUPS) + inner_ids).reshape(-1)
    flat_weights = route_weights.reshape(-1)
    room = N_EP * N_TP * CAP

    def one_expert(running, expert_num):
        matches = picks == expert_num
        picked = jnp.nonzero(matches, size=room, fill_value=0)[0].astype(jnp.int32)
        live = jnp.arange(room) < jnp.sum(matches)
        token_ids = picked // TOPK
        chosen_rows = normed[token_ids]
        gate_pre = jnp.dot(chosen_rows, gate_weight[expert_num], preferred_element_type=jnp.float32)
        up_pre = jnp.dot(chosen_rows, up_weight[expert_num], preferred_element_type=jnp.float32)
        hidden = (jax.nn.silu(gate_pre) * up_pre).astype(jnp.bfloat16)
        result = jnp.dot(hidden, down_weight[expert_num], preferred_element_type=jnp.float32).astype(jnp.bfloat16)
        weight_col = jnp.where(live, flat_weights[picked], jnp.float32(0.0))
        running = running.at[token_ids].add(result.astype(jnp.float32) * weight_col[:, None])
        return (running, None)
    running, _ = lax.scan(one_expert, jnp.zeros((TOKENS, D), jnp.float32), jnp.arange(EXPERTS, dtype=jnp.int32))
    combined = running.astype(jnp.bfloat16)
    return (attended, combined)
```

```python
import jax
import jax.numpy as jnp
from jax import lax
from jax.experimental import pallas as pl
from jax.experimental.pallas import tpu as pltpu
from jax.sharding import Mesh, PartitionSpec as P

GROUPS = 4
CAP = 10
EPS = 1e-06
NEG = -1e30
LOG2E = 1.4426950408889634


F32 = jnp.float32
BF16 = jnp.bfloat16
EP = ("z", "y", "c")


def dot(a, b):
    return jnp.dot(a, b, preferred_element_type=F32)


def dot_nt(a, b):
    return lax.dot_general(a, b, (((1,), (1,)), ((), ())), preferred_element_type=F32)


def dot_tn(a, b):
    return lax.dot_general(a, b, (((0,), (0,)), ((), ())), preferred_element_type=F32)


def vmem():
    return pl.BlockSpec(memory_space=pltpu.VMEM)


def smem():
    return pl.BlockSpec(memory_space=pltpu.SMEM)


def sds(shape, dtype=BF16):
    return jax.ShapeDtypeStruct(shape, dtype)


def kernel_call(fn, out_shape, in_specs, name, flops, scratch=(), nbytes=1 << 20):
    many = isinstance(out_shape, (list, tuple))
    return pl.pallas_call(
        fn,
        out_shape=out_shape,
        in_specs=in_specs,
        out_specs=[vmem() for _ in out_shape] if many else vmem(),
        scratch_shapes=list(scratch),
        name=name,
        cost_estimate=pl.CostEstimate(flops=flops, bytes_accessed=nbytes, transcendentals=0),
        compiler_params=pltpu.CompilerParams(vmem_limit_bytes=56 * 1024 * 1024),
    )


def iota(shape, dim):
    return lax.broadcasted_iota(jnp.int32, shape, dim)


QB = 512
KB = 1024


def attention_kernel(pos, q_early, q_late, kv, lam, gain, o_early, o_late, qs, acc, top):
    chip = pos[0]
    rows2 = 2 * QB

    def load_queries(q_ref):
        q = q_ref[...].astype(F32) * (0.125 * LOG2E)
        hi = q.astype(BF16)
        lo = (q - hi.astype(F32)).astype(BF16)
        both = jnp.concatenate([hi, lo], axis=1)
        lane = iota((QB, 256), 1)
        first = (lane % 128) < 64
        zero = jnp.zeros((QB, 256), BF16)
        qs[0:QB, :] = jnp.where(first, both, zero)
        qs[QB:rows2, :] = jnp.where(first, zero, both)

    def step(start, size, offset):
        k = kv[pl.ds(start, size), 0:128]
        v = kv[pl.ds(start, size), 128:256]
        kk = jnp.concatenate([k, k], axis=1)
        s = dot_nt(qs[...], kk)
        if offset is not None:
            row = iota((rows2, size), 0) % QB
            col = iota((rows2, size), 1)
            s = jnp.where(col <= row + offset, s, NEG)
        old = top[...]
        new = jnp.maximum(old, jnp.max(s, axis=1, keepdims=True))
        p = jnp.exp2(s - new[:, 0:1]).astype(BF16)
        fade = jnp.exp2(old - new)
        top[...] = new
        ones = jnp.ones((size, 128), BF16)
        vo = jnp.concatenate([v, ones], axis=1)
        acc[...] = acc[...] * fade[:, 0:1] + dot(p, vo)

    def group(q_ref, o_ref, chip_at, half):
        load_queries(q_ref)
        top[...] = jnp.full((rows2, 128), NEG, F32)
        acc[...] = jnp.zeros((rows2, 256), F32)

        def body(i, carry):
            step(pl.multiple_of(i * KB, KB), KB, None)
            return carry

        lax.fori_loop(0, chip_at, body, 0)
        step(pl.multiple_of(chip_at * KB, KB), QB * (half + 1), QB * half)
        out0 = acc[0:QB, 0:128] / acc[0:QB, 128:129]
        out1 = acc[QB:rows2, 0:128] / acc[QB:rows2, 128:129]
        head = out0 - lam[0, 0] * out1
        mean = jnp.mean(head * head, axis=1, keepdims=True)
        o_ref[...] = (head * lax.rsqrt(mean + EPS) * gain[...]).astype(BF16)

    group(q_early, o_early, chip, 0)
    group(q_late, o_late, 15 - chip, 1)


def attention(chip, q_early, q_late, kv, lam, gain):
    return kernel_call(
        attention_kernel,
        [sds((QB, 128)), sds((QB, 128))],
        [smem(), vmem(), vmem(), vmem(), smem(), vmem()],
        "attention",
        30_000_000_000,
        scratch=[
            pltpu.VMEM((2 * QB, 256), BF16),
            pltpu.VMEM((2 * QB, 256), F32),
            pltpu.VMEM((2 * QB, 128), F32),
        ],
    )(chip.reshape(1), q_early, q_late, kv, lam.reshape(1, 1), gain.reshape(1, 128))


GCAP = 4 * CAP
META = 128


def source_slots(gid, z):
    groups = iota((8, 128), 0)
    onehot = (gid == groups).astype(BF16)
    before = (iota((128, 128), 0) < iota((128, 128), 1)).astype(BF16)
    rank = dot(onehot, before).astype(jnp.int32)
    mine = jnp.sum(jnp.where(gid == groups, rank, 0), axis=0, keepdims=True)
    slot = ((gid - z) & 3) * GCAP + mine
    return (iota((4 * GCAP, 128), 0) == slot).astype(BF16)


def split3(w):
    hi = w.astype(BF16).astype(F32)
    mid = (w - hi).astype(BF16).astype(F32)
    low = (w - hi - mid).astype(BF16).astype(F32)
    return hi, mid, low


def prep_kernel(pos, tokens, gain, gid, inner, weights, *outs):
    wide = tokens[...].astype(F32)
    mean = jnp.mean(wide * wide, axis=1, keepdims=True)
    normed = (wide * lax.rsqrt(mean + EPS) * gain[...]).astype(BF16)
    place = source_slots(gid[...], pos[0])
    lane = iota((128, META), 1)
    ids = inner[...]
    columns = [(ids[:, 0:1] + 1).astype(F32), (ids[:, 1:2] + 1).astype(F32)]
    columns += list(split3(weights[:, 0:1])) + list(split3(weights[:, 1:2]))
    meta = jnp.zeros((128, META), F32)
    for at, column in enumerate(columns):
        meta = jnp.where(lane == at, column, meta)
    rows = dot(place, normed).astype(BF16)
    tags = dot(place, meta.astype(BF16)).astype(BF16)
    for d in range(4):
        outs[d][:, 0:2048] = rows[d * GCAP : (d + 1) * GCAP]
        outs[d][:, 2048 : 2048 + META] = tags[d * GCAP : (d + 1) * GCAP]


def dest_expert(j, y, c):
    return ((y + (j >> 1)) & 3) * 2 + (c ^ (j & 1))


def reslot_kernel(pos, r0, r1, r2, r3, *rest):
    outs, rows = rest[:8], rest[8]
    y, c = pos[1], pos[2]
    for d, r in enumerate((r0, r1, r2, r3)):
        rows[d * GCAP : (d + 1) * GCAP, :] = r[...]
    meta = rows[:, 2048 : 2048 + META]
    pick = (iota((8, META), 0) == iota((8, META), 1)).astype(BF16)
    ids = dot_nt(pick, meta).astype(jnp.int32)
    expert = dest_expert(iota((8, 160), 0), y, c) + 1
    hit = (ids[0:1] == expert) | (ids[1:2] == expert)
    before = (iota((160, 160), 0) < iota((160, 160), 1)).astype(BF16)
    rank = dot(hit.astype(BF16), before).astype(jnp.int32)
    rank = jnp.where(hit, rank, -1)
    slots = iota((GCAP, 160), 0)
    place = jnp.concatenate([(slots == rank[j : j + 1]).astype(BF16) for j in range(8)], axis=0)
    sent = dot(place, rows[:, 0:2048]).astype(BF16)
    for j in range(8):
        outs[j][...] = sent[j * GCAP : (j + 1) * GCAP]


def combine_kernel(pos, *refs):
    results, metas, outs, res = refs[:8], refs[8:12], refs[12:16], refs[16]
    y, c = pos[1], pos[2]
    for j in range(8):
        res[j * GCAP : (j + 1) * GCAP, :] = results[j][...]
    meta = jnp.concatenate([m[:, 2048 : 2048 + META] for m in metas], axis=0)
    wide = meta.astype(F32)
    id0 = wide[:, 0:1].astype(jnp.int32)
    id1 = wide[:, 1:2].astype(jnp.int32)
    w0 = wide[:, 2:3] + wide[:, 3:4] + wide[:, 4:5]
    w1 = wide[:, 5:6] + wide[:, 6:7] + wide[:, 7:8]
    j_at = iota((160, 128), 1)
    expert = jnp.where(j_at < 8, dest_expert(j_at, y, c) + 1, -1)
    hit0, hit1 = id0 == expert, id1 == expert
    before = (iota((160, 160), 1) < iota((160, 160), 0)).astype(BF16)
    rank = dot(before, (hit0 | hit1).astype(BF16)).astype(jnp.int32)
    slot = j_at * GCAP + rank
    slot0 = jnp.sum(jnp.where(hit0, slot + 1, 0), axis=1, keepdims=True) - 1
    slot1 = jnp.sum(jnp.where(hit1, slot + 1, 0), axis=1, keepdims=True) - 1
    at = iota((160, 320), 1)
    mix = jnp.where(at == slot0, w0, 0.0) + jnp.where(at == slot1, w1, 0.0)
    total = jnp.zeros((160, 2048), F32)
    for piece in split3(mix):
        total = total + dot(piece.astype(BF16), res[...])
    total = total.astype(BF16)
    for d in range(4):
        outs[d][...] = total[d * GCAP : (d + 1) * GCAP]


def unslot_kernel(pos, gid, c0, c1, c2, c3, out, rows):
    place = source_slots(gid[...], pos[0])
    for d, r in enumerate((c0, c1, c2, c3)):
        rows[d * GCAP : (d + 1) * GCAP, :] = r[...]
    out[...] = dot_tn(place, rows[...]).astype(BF16)


def hidden_kernel(x, g0, g1, u0, u1, out):
    rows = x[...]
    for at, (g, u) in enumerate(((g0, u0), (g1, u1))):
        gate = dot(rows, g[...])
        up = dot(rows, u[...])
        out[:, at * 256 : (at + 1) * 256] = (gate / (1.0 + jnp.exp(-gate)) * up).astype(BF16)


def down_kernel(h_own, h_got, d0, d1, d2, d3, *rest):
    outs, hid, wts = rest[:8], rest[8], rest[9]
    hid[:, 0:512] = h_own[...]
    hid[:, 512:1024] = h_got[...]
    for at, d in enumerate((d0, d1, d2, d3)):
        wts[at * 256 : (at + 1) * 256, :] = d[...]
    res = dot(hid[...], wts[...]).astype(BF16)
    for j in range(8):
        outs[j][...] = res[j * GCAP : (j + 1) * GCAP]


def project_kernel(pos, h0, h1, h2, h3, weight, out):
    x = pos[3]
    total = jnp.zeros((128, 2048), F32)
    for d, h in enumerate((h0, h1, h2, h3)):
        w = weight[:, (x - d) & 3].reshape(256, 2048)
        total = total + dot(h[...], w)
    out[...] = total.astype(BF16)


def ring(d):
    return [(i, (i + d) % 4) for i in range(4)]


def yc_perm(j):
    return [(i, ((i // 2 + j // 2) % 4) * 2 + ((i % 2) ^ (j % 2))) for i in range(8)]


def yc_back(j):
    return [(b, a) for a, b in yc_perm(j)]


def body(
    query_rows,
    key_rows,
    value_rows,
    lambdas,
    out_gain,
    out_weight,
    tokens,
    norm_gain,
    group_ids,
    inner_ids,
    route_weights,
    gate_weight,
    up_weight,
    down_weight,
):
    z = lax.axis_index("z")
    y = lax.axis_index("y")
    c = lax.axis_index("c")
    x = lax.axis_index("x")
    chip = z * 4 + y
    pos = jnp.stack([z, y, c, x]).astype(jnp.int32)
    even = c == 0

    gid = group_ids.reshape(1, 128)
    outgoing = kernel_call(
        prep_kernel,
        [sds((GCAP, 2048 + META))] * 4,
        [smem()] + [vmem()] * 5,
        "prep",
        100_000_000,
    )(pos, tokens, norm_gain.reshape(1, 2048), gid, inner_ids, route_weights)
    planes = [outgoing[0]] + [lax.ppermute(outgoing[d], "z", ring(d)) for d in (1, 2, 3)]

    def head_of(rows, which):
        return jnp.where(which, rows[:, 0:128], rows[:, 128:256])

    kv_mine = jnp.concatenate([head_of(key_rows, even), head_of(value_rows, even)], axis=1)
    kv_send = jnp.concatenate([head_of(key_rows, ~even), head_of(value_rows, ~even)], axis=1)
    kv_got = lax.ppermute(kv_send, "c", [(0, 1), (1, 0)])
    kv_chip = jnp.concatenate(
        [jnp.where(even, kv_mine, kv_got), jnp.where(even, kv_got, kv_mine)], axis=0
    )
    kv_all = lax.all_gather(kv_chip, ("z", "y"), axis=0, tiled=True)

    q_mine, q_send = head_of(query_rows, even), head_of(query_rows, ~even)
    mirror = lambda p: 15 - p
    perm1 = [(2 * p, 2 * p + 1) for p in range(16)]
    perm1 += [(2 * p + 1, 2 * mirror(p)) for p in range(16)]
    perm2 = [(2 * p + 1, 2 * mirror(p) + 1) for p in range(16)]
    q_got1 = lax.ppermute(q_send, EP, perm1)
    q_got2 = lax.ppermute(q_mine, EP, perm2)
    q_early = jnp.where(even, q_mine, q_got1)
    q_late = jnp.where(even, q_got1, q_got2)

    pair = [(i, i ^ 1) for i in range(4)]
    cross = [(i, 3 - i) for i in range(4)]
    gate0, up0, down0 = gate_weight[0], up_weight[0], down_weight[0]
    down1 = lax.ppermute(down0, "x", pair)
    gate1 = lax.ppermute(gate0, "x", pair)
    up1 = lax.ppermute(up0, "x", pair)
    down2 = lax.ppermute(down0, "x", cross)
    down3 = lax.ppermute(down1, "x", cross)

    ep = chip * 2 + c
    piece = lax.dynamic_slice_in_dim(out_weight, ep * 8, 8, 0)
    weight_all = lax.all_gather(piece, ("z", "y", "c", "x"), axis=0, tiled=True)
    weight_all = weight_all.reshape(32, 4, 8, 2048)

    slots = kernel_call(
        reslot_kernel,
        [sds((GCAP, 2048))] * 8,
        [smem()] + [vmem()] * 4,
        "reslot",
        300_000_000,
        scratch=[pltpu.VMEM((4 * GCAP, 2048 + META), BF16)],
    )(pos, *planes)
    rows = [slots[0]] + [lax.ppermute(slots[j], ("y", "c"), yc_perm(j)) for j in range(1, 8)]
    rows_mine = jnp.concatenate(rows, axis=0)
    rows_got = lax.ppermute(rows_mine, "x", cross)

    def hidden(rows):
        return kernel_call(
            hidden_kernel,
            sds((8 * GCAP, 512)),
            [vmem()] * 5,
            "hidden",
            1_300_000_000,
        )(rows, gate0, gate1, up0, up1)

    hid_send = hidden(rows_got)
    hid_got = lax.ppermute(hid_send, "x", cross)
    hid_own = hidden(rows_mine)
    results = kernel_call(
        down_kernel,
        [sds((GCAP, 2048))] * 8,
        [vmem()] * 6,
        "down",
        1_300_000_000,
        scratch=[pltpu.VMEM((320, 1024), BF16), pltpu.VMEM((1024, 2048), BF16)],
    )(hid_own, hid_got, down0, down1, down2, down3)
    returned = [results[0]] + [
        lax.ppermute(results[j], ("y", "c"), yc_back(j)) for j in range(1, 8)
    ]
    mixed = kernel_call(
        combine_kernel,
        [sds((GCAP, 2048))] * 4,
        [smem()] + [vmem()] * 12,
        "combine",
        700_000_000,
        scratch=[pltpu.VMEM((8 * GCAP, 2048), BF16)],
    )(pos, *returned, *planes)
    back = [mixed[0]] + [lax.ppermute(mixed[d], "z", ring(4 - d)) for d in (1, 2, 3)]
    combined = kernel_call(
        unslot_kernel,
        sds((128, 2048)),
        [smem()] + [vmem()] * 5,
        "unslot",
        100_000_000,
        scratch=[pltpu.VMEM((4 * GCAP, 2048), BF16)],
    )(pos, gid, *back)

    lam = jnp.where(even, lambdas[0], lambdas[1])
    o_early, o_late = attention(chip, q_early, q_late, kv_all, lam, out_gain)
    perm3 = [(2 * p, 2 * mirror(p) + 1) for p in range(16)]
    perm3 += [(2 * p + 1, 2 * p) for p in range(16)]
    o_got1 = lax.ppermute(jnp.where(even, o_late, o_early), EP, perm3)
    o_got2 = lax.ppermute(o_late, EP, perm2)
    heads = jnp.concatenate(
        [jnp.where(even, o_early, o_got1), jnp.where(even, o_got1, o_got2)], axis=1
    )
    parts = []
    for d in range(4):
        block = lax.dynamic_slice_in_dim(heads, ((x + d) & 3) * 128, 128, 0)
        parts.append(lax.ppermute(block, "x", ring(d)) if d else block)
    attended = kernel_call(
        project_kernel,
        sds((128, 2048)),
        [smem()] + [vmem()] * 5,
        "project",
        540_000_000,
    )(pos, *parts, weight_all)
    return (attended, combined)


def solution(mesh):
    fine = Mesh(mesh.devices.reshape(4, 4, 2, 4), ("z", "y", "c", "x"))
    every = ("z", "y", "c", "x")
    in_specs = (
        P(EP, "x"),
        P(EP, "x"),
        P(EP, "x"),
        P("x"),
        P(),
        P("x", None),
        P(every, None),
        P(),
        P(every),
        P(every, None),
        P(every, None),
        P(EP, None, "x"),
        P(EP, None, "x"),
        P(EP, "x", None),
    )
    out_specs = (P(every, None), P(every, None))
    return jax.shard_map(body, mesh=fine, in_specs=in_specs, out_specs=out_specs, check_vma=False)
```
